32 devices in a mesh: sp: 8 (over z, x), tp: 4 (over y, core).
Axes of the slice: x: 2, y: 2, z: 4, core: 2. Of those that a mesh axis runs over, the one named last changes fastest.
Arguments:
- queries: bfloat16 [2048, 2048], P('sp', 'tp'), may hold values from -100 to 100
- key_columns: bfloat16 [1024, 2048], P('tp', 'sp'), may hold values from -24 to 24
- value_columns: bfloat16 [1024, 2048], P('tp', 'sp'), may hold values from -24 to 24
- sink_logits: float32 [32], P('tp'), may hold values from 3 to 7
- out_weight: bfloat16 [2048, 2048], P('tp'), may hold values from -0.1875 to 0.1875
- stream_in: bfloat16 [2048, 2048], P('sp'), may hold values from -3 to 3
- norm_gain: float32 [2048], replicated, may hold values from 0.1 to 1.9
- expert_ids: int32 [2048, 2], P('sp'), may hold values from 0 to 7, all different within a row; in each aligned block of 256 rows (0 to 255, 256 to 511, ...) at most 128 rows name the same one
- route_weights: float32 [2048, 2], P('sp'), may hold values from 0.1 to 0.7
- gate_weight: bfloat16 [8, 2048, 4096], P('sp', None, 'tp'), may hold values from -0.125 to 0.125
- up_weight: bfloat16 [8, 2048, 4096], P('sp', None, 'tp'), may hold values from -0.125 to 0.125
- down_weight: bfloat16 [8, 4096, 2048], P('sp', 'tp'), may hold values from -0.125 to 0.125
Outputs:
- layer_out: bfloat16 [2048, 2048], P('sp', 'tp')
The draws below stay inside these ranges and needn't reach their ends.
Inputs may be any that keep to these rules, and one draw needn't show every extreme that they name: `expert_ids`: each row names 2 different experts. In each aligned block of 256 tokens no expert is named by more than 128 rows, and in some blocks one expert is named by exactly 128 rows.
All inputs are finite; a program needn't handle non-finite values.
Results may differ from the reference program's by a relative error of at most 0.02.
Values may be sent and summed in bfloat16 or wider, within the bound.
A program may use at most 64 MiB of HBM per device.

```python
import math
import jax
import jax.numpy as jnp
import numpy as np
from jax import lax

D = 2048
QH = 32
KVH = 16
HD = 64
FFE = 4096
WINDOW = 128
TOP = 2
T_SP = 256
TOKENS = 2048
EXPERTS = 8
CAP = 128
N_SP = 8
N_TP = 4


def draw_queries(key, part):
    drawn = jnp.clip(jax.random.normal(jax.random.fold_in(key, 1), (TOKENS, QH * HD), jnp.float32), -6.0, 6.0)
    return drawn.astype(jnp.bfloat16)


def draw_key_columns(key, part):
    drawn = jnp.clip(jax.random.normal(jax.random.fold_in(key, 2), (KVH * HD, TOKENS), jnp.float32), -6.0, 6.0)
    return drawn.astype(jnp.bfloat16)


def strengthened(drawn, stream_key, source, target, shards_of, factor):
    def block_of(dim):
        return (jnp.arange(drawn.shape[dim]) // (drawn.shape[dim] // shards_of)).reshape((-1,) + (1,) * (drawn.ndim - 1 - dim))

    first = jax.random.permutation(stream_key, shards_of)[block_of(target)]
    second = (block_of(target) + shards_of // 2) % shards_of
    return jnp.where((block_of(source) == first) | (block_of(source) == second), factor * drawn, drawn)


def shard_levels(stream_key, dims, cuts, smallest, largest):
    def one(dim, shards_of):
        heights = jax.random.uniform(jax.random.fold_in(jax.random.fold_in(stream_key, 6), dim), (shards_of,), jnp.float32, smallest / len(cuts), largest / len(cuts))
        return jnp.repeat(jnp.exp(heights), dims[dim] // shards_of).reshape((-1,) + (1,) * (len(dims) - dim - 1))

    gain = one(*cuts[0])
    for cut in cuts[1:]:
        gain = gain * one(*cut)
    return gain


def routed_block(key, own, number, rows, amount, top, bound, lean):
    order = jax.random.permutation(key, amount)
    heavy_load, usual = load_shares(amount, rows * top, bound, lean, True), load_shares(amount, rows * top, bound, lean, False)
    places = jnp.arange(amount)

    def named(tallies, turn):
        used = int((tallies > 0).sum())
        fixed = max(1, used // 4)
        moved = fixed + (places - fixed + turn * (used - fixed)) % max(1, amount - fixed)
        return jnp.zeros((amount,), jnp.int32).at[order[jnp.where(places < fixed, places, moved)]].set(jnp.asarray(tallies, jnp.int32))

    tallies = jnp.where(number % 4 == 0, named(heavy_load, number // 4), named(usual, number - number // 4 - 1))
    mixed = jax.random.permutation(jax.random.fold_in(own, 3), amount)
    donor, sink = mixed[0:amount // 2 * 2:2], mixed[1:amount // 2 * 2:2]
    slack = jnp.minimum(tallies[donor] - 1, bound - tallies[sink]) // 2
    slack = jnp.where((donor == order[0]) | (sink == order[0]) | (tallies[sink] == 0), 0, jnp.maximum(slack, 0))
    moved = jax.random.randint(jax.random.fold_in(own, 4), (amount // 2,), 0, 1 << 20) % (slack + 1)
    tallies = tallies.at[donor].add(-moved).at[sink].add(moved)
    items = jnp.searchsorted(jnp.cumsum(tallies), jnp.arange(rows * top), side="right").astype(jnp.int32)
    table = items.reshape(top, rows).T
    table = table[jax.random.permutation(jax.random.fold_in(own, 1), rows)]
    turn = jax.random.randint(jax.random.fold_in(own, 2), (rows, 1), 0, top)
    return jnp.take_along_axis(table, (jnp.arange(top)[None, :] + turn) % top, axis=1)


def load_shares(amount, total, most, skew, full):
    loads = [(1 << 20) // math.isqrt(rank ** skew) + 1 for rank in range(1, amount + 1)]
    largest = most if full else min(most, max(-(-total // amount), total * loads[0] // sum(loads)))
    least = 1 if total - largest >= amount - 1 else 0
    counts, spare = [largest] + [least] * (amount - 1), total - largest - least * (amount - 1)
    while spare > 0:
        movable = [i for i in range(1, amount) if counts[i] < largest] or [i for i in range(1, amount) if counts[i] < most]
        mass, remaining = sum([loads[i] for i in movable]), spare
        for i in movable:
            extra = min(most - counts[i], max(1, remaining * loads[i] // mass), spare)
            counts[i] = counts[i] + extra
            spare = spare - extra
    return np.array(counts)


def centred(own_key, dims, deviation, most, pieces=(), held_as=jnp.bfloat16):
    drawn = deviation * jax.random.normal(own_key, dims, jnp.float32)
    if pieces:
        drawn = drawn * shard_levels(own_key, dims, pieces, -0.22, 0.18)
    return jnp.clip(drawn, -most, most).astype(held_as)


def bell_draw_with(rng, dims, spread, most, cuts, heavy, kind=jnp.bfloat16):
    values = spread * jax.random.normal(rng, dims, jnp.float32)
    if cuts:
        values = values * shard_levels(rng, dims, cuts, -0.22, 0.18)
    return jnp.clip(strengthened(values, jax.random.fold_in(rng, 3), *heavy), -most, most).astype(kind)


def setup_inputs(seed: int = 0) -> dict:
    key_of = jax.random.split(jax.random.key(seed), 13)
    queries = draw_queries(jax.random.fold_in(key_of[12], 71), 0)
    key_columns = draw_key_columns(jax.random.fold_in(key_of[12], 71), 0)
    value_columns = centred(key_of[2], (KVH * HD, TOKENS), 4.0, 24.0, ((0, 4), (1, 8)))
    sink_logits = jnp.clip(3.0 + 4.0 * jax.random.uniform(key_of[3], (QH,), jnp.float32) ** shard_levels(key_of[3], (QH,), ((0, 4),), -0.2, 0.2), 3.0, 7.0)
    out_weight = bell_draw_with(key_of[4], (QH * HD, D), (QH * HD) ** -0.5, 0.1875, ((0, 4),), (0, 1, 4, 2.0))
    stream_in = centred(key_of[5], (TOKENS, D), 0.5, 3.0, ((0, 8),))
    norm_gain = jnp.clip(1.0 + 0.18 * jax.random.normal(key_of[6], (D,), jnp.float32), 0.1, 1.9)
    expert_ids_keys = jax.random.split(jax.random.fold_in(key_of[7], 1), TOKENS // T_SP)
    expert_ids_turns = jax.random.permutation(jax.random.fold_in(key_of[7], 3), TOKENS // T_SP)
    expert_ids = jax.vmap(lambda own, number: routed_block(jax.random.fold_in(key_of[7], 2), own, number, T_SP, EXPERTS, TOP, CAP, 1))(expert_ids_keys, expert_ids_turns).reshape((TOKENS, TOP))
    route_weights = jnp.clip(0.1 + 0.59999999 * jax.random.uniform(key_of[8], (TOKENS, TOP), jnp.float32) ** shard_levels(key_of[8], (TOKENS, TOP), ((0, 8),), -0.2, 0.2), 0.1, 0.7)
    gate_weight = centred(key_of[9], (EXPERTS, D, FFE), D ** -0.5, 0.125, ((0, 8), (2, 4)))
    up_weight = centred(key_of[10], (EXPERTS, D, FFE), D ** -0.5, 0.125, ((0, 8), (2, 4)))
    down_weight = bell_draw_with(key_of[11], (EXPERTS, FFE, D), FFE ** -0.5, 0.125, ((0, 8), (1, 4)), (1, 2, 4, 2.0))
    return {"queries": queries, "key_columns": key_columns, "value_columns": value_columns, "sink_logits": sink_logits, "out_weight": out_weight, "stream_in": stream_in, "norm_gain": norm_gain, "expert_ids": expert_ids, "route_weights": route_weights, "gate_weight": gate_weight, "up_weight": up_weight, "down_weight": down_weight}


EPSILON = 1e-06
MASKED = -1e+30

def rounded(number):
    return lax.optimization_barrier(number.astype(jnp.bfloat16)).astype(jnp.float32)

def rms_scale(residual, norm_gain):
    widened = residual.astype(jnp.float32)
    inverse_rms = lax.rsqrt(lax.optimization_barrier(jnp.mean(widened * widened, axis=-1, keepdims=True)) + EPSILON)
    return (widened * inverse_rms * norm_gain.astype(jnp.float32)).astype(jnp.bfloat16)

def attend(queries, key_columns, value_columns, sink_logits):
    per_group = QH // KVH
    blocks = TOKENS // WINDOW
    key_span = 3 * WINDOW
    padding = jnp.zeros((KVH * HD, WINDOW), jnp.bfloat16)
    key_padded = jnp.concatenate([padding, key_columns, padding], axis=1)
    value_padded = jnp.concatenate([padding, value_columns, padding], axis=1)
    query_blocks = queries.reshape(blocks, WINDOW, KVH, per_group, HD)
    sink_logit = sink_logits.astype(jnp.float32).reshape(KVH, per_group)[:, :, None]

    def one_block(block_index):
        offset = (block_index * WINDOW).astype(jnp.int32)
        query_block = lax.dynamic_index_in_dim(query_blocks, block_index, 0, keepdims=False).astype(jnp.float32)
        key_block = lax.dynamic_slice_in_dim(key_padded, offset, key_span, 1).reshape(KVH, HD, key_span).astype(jnp.float32)
        value_block = lax.dynamic_slice_in_dim(value_padded, offset, key_span, 1).reshape(KVH, HD, key_span).astype(jnp.float32)
        scores = jnp.einsum('qkgd,kdj->kgqj', query_block, key_block) / math.sqrt(HD)
        query_pos = offset + jnp.arange(WINDOW, dtype=jnp.int32)
        key_pos = offset - WINDOW + jnp.arange(key_span, dtype=jnp.int32)
        visible = (jnp.abs(query_pos[:, None] - key_pos[None, :]) <= WINDOW) & (key_pos >= 0)[None, :] & (key_pos < TOKENS)[None, :]
        scores = jnp.where(visible, scores, MASKED)
        row_top = jnp.maximum(lax.optimization_barrier(jnp.max(scores, axis=-1)), sink_logit)
        exponent = jnp.where(visible, jnp.exp(scores - row_top[..., None]), 0.0)
        denominator = lax.optimization_barrier(jnp.sum(exponent, axis=-1)) + jnp.exp(sink_logit - row_top)
        attn_weights = (exponent / denominator[..., None]).astype(jnp.bfloat16)
        head_mix = jnp.einsum('kgqj,kdj->qkgd', attn_weights.astype(jnp.float32), value_block)
        return head_mix.reshape(WINDOW, QH * HD).astype(jnp.bfloat16)
    return lax.map(one_block, jnp.arange(blocks, dtype=jnp.int32)).reshape(TOKENS, QH * HD)

def project_heads(head_out, out_weight):
    group_width = QH * HD // N_TP

    def add_group(carry, group_index):
        offset = (group_index * group_width).astype(jnp.int32)
        head_piece = lax.dynamic_slice_in_dim(head_out, offset, group_width, 1)
        weight_rows = lax.dynamic_slice_in_dim(out_weight, offset, group_width, 0)
        return (carry + rounded(jnp.dot(head_piece, weight_rows, preferred_element_type=jnp.float32)), None)
    summed, unused = lax.scan(add_group, jnp.zeros((TOKENS, D), jnp.float32), jnp.arange(N_TP, dtype=jnp.int32))
    return summed

def one_expert(operands):
    expert_rows_in, gate_matrix, up_matrix, down_matrix = operands
    gate_pre = jnp.dot(expert_rows_in, gate_matrix, preferred_element_type=jnp.float32)
    upward = jnp.dot(expert_rows_in, up_matrix, preferred_element_type=jnp.float32)
    hidden = (jax.nn.silu(gate_pre) * upward).astype(jnp.bfloat16)
    group_width = FFE // N_TP

    def add_group(carry, group_index):
        offset = (group_index * group_width).astype(jnp.int32)
        hidden_piece = lax.dynamic_slice_in_dim(hidden, offset, group_width, 1)
        down_rows = lax.dynamic_slice_in_dim(down_matrix, offset, group_width, 0)
        return (carry + rounded(jnp.dot(hidden_piece, down_rows, preferred_element_type=jnp.float32)), None)
    summed, unused = lax.scan(add_group, jnp.zeros((expert_rows_in.shape[0], D), jnp.float32), jnp.arange(N_TP, dtype=jnp.int32))
    return summed.astype(jnp.bfloat16)

def reference(queries, key_columns, value_columns, sink_logits, out_weight, stream_in, norm_gain, expert_ids, route_weights, gate_weight, up_weight, down_weight):
    head_out = attend(queries, key_columns, value_columns, sink_logits)
    attn_sum = project_heads(head_out, out_weight)
    residual = (stream_in.astype(jnp.float32) + rounded(attn_sum)).astype(jnp.bfloat16)
    normed = rms_scale(residual, norm_gain)
    route_ids = expert_ids.reshape(N_SP, T_SP * TOP)
    route_hits = (route_ids[..., None] == jnp.arange(EXPERTS, dtype=jnp.int32)).astype(jnp.int32)
    earlier = jnp.cumsum(route_hits, axis=1) - route_hits
    slot_index = lax.optimization_barrier(jnp.sum(earlier * route_hits, axis=2)).astype(jnp.int32)
    source = jnp.broadcast_to(jnp.arange(N_SP, dtype=jnp.int32)[:, None], route_ids.shape)
    position = source * CAP + slot_index
    route_rows = jnp.repeat(normed.reshape(N_SP, T_SP, 1, D), TOP, axis=2).reshape(N_SP, T_SP * TOP, D)
    buffer = jnp.zeros((EXPERTS, N_SP * CAP, D), jnp.bfloat16).at[route_ids, position].set(route_rows)
    expert_out = lax.map(one_expert, (buffer, gate_weight, up_weight, down_weight))
    picked = expert_out[route_ids, position].reshape(TOKENS, TOP, D).astype(jnp.float32)
    expert_sum = lax.optimization_barrier(jnp.sum(picked * route_weights[:, :, None], axis=1))
    return (residual.astype(jnp.float32) + expert_sum).astype(jnp.bfloat16)
```

```python
import functools
import math

import jax
import jax.numpy as jnp
from jax import lax
from jax.experimental import pallas as pl
from jax.experimental.pallas import tpu as pltpu
from jax.sharding import PartitionSpec as P

HD = 64
WINDOW = 128
CORES = 2
EPSILON = 1e-06
MASKED = -1e30
MESH = pl.DeviceIdType.MESH
F32 = jnp.float32
BF16 = jnp.bfloat16


def iota(shape, dim):
    return lax.broadcasted_iota(jnp.int32, shape, dim)


def dot(a, b):
    return jnp.dot(a, b, preferred_element_type=F32)


def as_row(column):
    size = column.shape[0]
    eye = iota((size, size), 0) == iota((size, size), 1)
    return jnp.sum(jnp.where(eye, column, 0.0), axis=0, keepdims=True)


def as_column(row):
    size = row.shape[1]
    eye = iota((size, size), 0) == iota((size, size), 1)
    return jnp.sum(jnp.where(eye, row, 0.0), axis=1, keepdims=True)


def send(src, dst, send_sem, recv_sem, device):
    copy = pltpu.make_async_remote_copy(
        src_ref=src,
        dst_ref=dst,
        send_sem=send_sem,
        recv_sem=recv_sem,
        device_id=device,
        device_id_type=MESH,
    )
    copy.start()


def sent(ref, sem, device):
    pltpu.make_async_remote_copy(
        src_ref=ref, dst_ref=ref, send_sem=sem, recv_sem=sem,
        device_id=device, device_id_type=MESH,
    ).wait_send()


def landed(ref, sem, device):
    pltpu.make_async_remote_copy(
        src_ref=ref, dst_ref=ref, send_sem=sem, recv_sem=sem,
        device_id=device, device_id_type=MESH,
    ).wait_recv()


def layer(
    n, tp, cap,
    q_ref, k_ref, v_ref, sink_ref, gain_ref, ids_ref, rw_ref,
    ow_hbm, stream_hbm, gate_hbm, up_hbm, down_hbm,
    out_ref,
    ow, stream, gate, up, down,
    halo, head, part, part_in, part_sum, part_y, squares,
    slots, xb, hid, po, po_in, chip_sum, sum_y, final, back, residual,
    load_sem, halo_send, halo_recv, ps_send, ps_recv, py_send, py_recv, sq_send, sq_recv,
    d_send, x_recv, fc_send, fy_send, f2_send,
    po_send, po_recv, y_send, y_recv, r_send, r_recv,
):
    s, t = lax.axis_index("sp"), lax.axis_index("tp")
    ny = tp // CORES
    y, c = t // CORES, lax.rem(t, CORES)
    other = 1 - c
    tok, width = residual.shape
    hidden = gate.shape[1]

    def at_sp(i):
        return (i, t)

    def at_tp(j):
        return (s, j)

    partner = at_tp(y * CORES + other)

    def peer_y(dy):
        return lax.rem(y + dy, ny)

    def from_y(dy):
        return lax.rem(y + ny - dy, ny)

    loads = [
        pltpu.make_async_copy(ow_hbm, ow, load_sem.at[0]),
        pltpu.make_async_copy(
            stream_hbm.at[:, pl.ds(pl.multiple_of(t * width, 128), width)], stream, load_sem.at[1]
        ),
        pltpu.make_async_copy(gate_hbm.at[0], gate, load_sem.at[2]),
        pltpu.make_async_copy(up_hbm.at[0], up, load_sem.at[3]),
        pltpu.make_async_copy(down_hbm.at[0], down, load_sem.at[4]),
    ]
    for load in loads:
        load.start()

    barrier = pltpu.get_barrier_semaphore()

    def greet_sp(i, _):
        pl.semaphore_signal(
            barrier, inc=1, device_id=at_sp(lax.rem(s + i, n)), device_id_type=MESH
        )
        return 0

    def greet_tp(j, _):
        pl.semaphore_signal(
            barrier, inc=1, device_id=at_tp(lax.rem(t + j, tp)), device_id_type=MESH
        )
        return 0

    lax.fori_loop(1, n, greet_sp, 0)
    lax.fori_loop(1, tp, greet_tp, 0)
    pl.semaphore_wait(barrier, n - 1 + tp - 1)

    right, left = at_sp(lax.rem(s + 1, n)), at_sp(lax.rem(s + n - 1, n))
    for a, source in enumerate((k_ref, v_ref)):
        send(source.at[:, pl.ds(tok - WINDOW, WINDOW)], halo.at[a, 0],
             halo_send.at[a, 0], halo_recv.at[a, 0], right)
        send(source.at[:, pl.ds(0, WINDOW)], halo.at[a, 1],
             halo_send.at[a, 1], halo_recv.at[a, 1], left)

    experts = n
    ids = ids_ref[...]
    lanes = iota((tok, 128), 1)
    top = ids.shape[1]
    hits = [(lanes == ids[:, k : k + 1]).astype(F32) for k in range(top)]
    all_hits = functools.reduce(jnp.add, hits)
    before = (iota((tok, tok), 1) < iota((tok, tok), 0)).astype(BF16)
    earlier = dot(before, all_hits.astype(BF16))
    place = [
        jnp.sum(earlier * hits[k], axis=1, keepdims=True) + ids[:, k : k + 1].astype(F32) * cap
        for k in range(top)
    ]
    place_row = [as_row(p) for p in place]

    for a, source in enumerate((k_ref, v_ref)):
        landed(halo.at[a, 0], halo_recv.at[a, 0], left)
        landed(halo.at[a, 1], halo_recv.at[a, 1], right)

    kv_heads = k_ref.shape[0] // HD
    group = q_ref.shape[1] // HD // kv_heads
    span = 3 * WINDOW
    row = lax.rem(iota((group * WINDOW, span), 0), WINDOW)
    col = iota((group * WINDOW, span), 1)
    near = (col - row >= 0) & (col - row <= 2 * WINDOW)
    for b in range(tok // WINDOW):
        key_pos = s * tok + (b - 1) * WINDOW + col
        visible = near & (key_pos >= 0) & (key_pos < n * tok)
        rows = pl.ds(b * WINDOW, WINDOW)
        for g in range(kv_heads):
            feats = pl.ds(g * HD, HD)
            kx, vx = [
                jnp.concatenate(
                    [halo[a, 0, feats, :], ref[feats, :], halo[a, 1, feats, :]], axis=1
                )[:, b * WINDOW : b * WINDOW + span]
                for a, ref in enumerate((k_ref, v_ref))
            ]
            qs = jnp.concatenate(
                [q_ref[rows, pl.ds((g * group + h) * HD, HD)] for h in range(group)], axis=0
            )
            sink = jnp.concatenate(
                [jnp.full((WINDOW, 1), sink_ref[g * group + h], F32) for h in range(group)], axis=0
            )
            scores = jnp.where(visible, dot(qs, kx) * (1.0 / math.sqrt(HD)), MASKED)
            row_top = jnp.maximum(jnp.max(scores, axis=1, keepdims=True), sink)
            weight = jnp.where(visible, jnp.exp(scores - row_top), 0.0)
            total = jnp.sum(weight, axis=1, keepdims=True) + jnp.exp(sink - row_top)
            weight = (weight * (1.0 / total)).astype(BF16)
            mixed = lax.dot_general(
                weight, vx, (((1,), (1,)), ((), ())), preferred_element_type=F32
            ).astype(BF16)
            head[rows, pl.ds(g * group * HD, group * HD)] = jnp.concatenate(
                [mixed[h * WINDOW : (h + 1) * WINDOW] for h in range(group)], axis=1
            )

    loads[0].wait()
    loads[1].wait()

    def project(core):
        for yy in range(ny):
            start = pl.multiple_of((yy * CORES + core) * width, 128)
            part[core, yy] = dot(head[...], ow[:, pl.ds(start, width)]).astype(BF16)

    project(other)
    send(part.at[other], part_in, ps_send, ps_recv, partner)
    project(c)
    landed(part_in, ps_recv, partner)
    for dy in range(1, ny):
        yy = peer_y(dy)
        part_sum[dy] = (part[c, yy].astype(F32) + part_in[yy].astype(F32)).astype(BF16)
        send(part_sum.at[dy], part_y.at[dy], py_send.at[dy], py_recv.at[dy],
             at_tp(yy * CORES + c))
    attn = part[c, y].astype(F32) + part_in[y].astype(F32)
    for dy in range(1, ny):
        landed(part_y.at[dy], py_recv.at[dy], at_tp(from_y(dy) * CORES + c))
        attn = attn + part_y[dy].astype(F32)
    res = (stream[...].astype(F32) + attn.astype(BF16).astype(F32)).astype(BF16)
    residual[...] = res
    res = res.astype(F32)
    own_squares = jnp.broadcast_to(as_row(jnp.sum(res * res, axis=1, keepdims=True)), (8, tok))
    squares[0] = own_squares
    for dt in range(1, tp):
        send(squares.at[0], squares.at[dt], sq_send.at[dt], sq_recv.at[dt],
             at_tp(lax.rem(t + dt, tp)))
    square_sum = own_squares
    for dt in range(1, tp):
        landed(squares.at[dt], sq_recv.at[dt], at_tp(lax.rem(t + tp - dt, tp)))
        square_sum = square_sum + squares[dt]
    inverse = as_column(lax.rsqrt(square_sum[0:1] / (tp * width) + EPSILON))
    gain = gain_ref[:, pl.ds(pl.multiple_of(t * width, 128), width)]
    normed = (res * inverse * gain).astype(BF16)

    slot = iota((cap, tok), 0)

    def rows_of(e):
        wanted = (slot + e * cap).astype(F32)
        pick = functools.reduce(jnp.logical_or, [wanted == p for p in place_row])
        return dot(pick.astype(F32).astype(BF16), normed).astype(BF16)

    xb[t, s] = rows_of(s)

    def dispatch(i, _):
        e = lax.rem(s + i, n)
        slots[i] = rows_of(e)
        send(slots.at[i], xb.at[t, s], d_send.at[i], x_recv.at[t, s], at_sp(e))
        return 0

    lax.fori_loop(1, n, dispatch, 0)
    for load in loads[2:]:
        load.wait()

    def forward(i):
        src = lax.rem(s + n - i, n)

        @pl.when(i > 0)
        def _():
            landed(xb.at[t, src], x_recv.at[t, src], at_sp(src))

        for dy in range(1, ny):
            send(xb.at[t, src], xb.at[t, src], fy_send.at[dy, i], x_recv.at[t, src],
                 at_tp(peer_y(dy) * CORES + c))
        send(xb.at[t, src], xb.at[t, src], fc_send.at[i], x_recv.at[t, src], partner)

    def relay(i):
        src = lax.rem(s + n - i, n)
        for dy in range(1, ny):
            j = from_y(dy) * CORES + c
            landed(xb.at[j, src], x_recv.at[j, src], at_tp(j))
            send(xb.at[j, src], xb.at[j, src], f2_send.at[dy, i], x_recv.at[j, src], partner)

    tile = min(hidden, 256)

    def expert(i):
        src = lax.rem(s + n - i, n)
        for yy in range(ny):
            j = yy * CORES + other
            landed(xb.at[j, src], x_recv.at[j, src], partner)
        rows = jnp.concatenate([xb[j, src] for j in range(tp)], axis=1)
        for f in range(hidden // tile):
            cols = pl.ds(f * tile, tile)
            gate_pre = dot(rows, gate[:, cols])
            upward = dot(rows, up[:, cols])
            hid[:, cols] = (gate_pre / (1.0 + jnp.exp(-gate_pre)) * upward).astype(BF16)
        for j in range(tp):
            po[i, j % CORES, j // CORES] = dot(
                hid[...], down[:, j * width : (j + 1) * width]
            ).astype(BF16)
        send(po.at[i, other], po_in.at[i], po_send.at[i], po_recv.at[i], partner)

    def chip_add(i):
        landed(po_in.at[i], po_recv.at[i], partner)
        for dy in range(1, ny):
            yy = peer_y(dy)
            chip_sum[dy, i] = (po[i, c, yy].astype(F32) + po_in[i, yy].astype(F32)).astype(BF16)
            send(chip_sum.at[dy, i], sum_y.at[dy, i], y_send.at[dy, i], y_recv.at[dy, i],
                 at_tp(yy * CORES + c))

    def finish(i):
        src = lax.rem(s + n - i, n)
        total = po[i, c, y].astype(F32) + po_in[i, y].astype(F32)
        for dy in range(1, ny):
            landed(sum_y.at[dy, i], y_recv.at[dy, i], at_tp(from_y(dy) * CORES + c))
            total = total + sum_y[dy, i].astype(F32)

        @pl.when(i == 0)
        def _():
            back[s] = total.astype(BF16)

        @pl.when(i > 0)
        def _():
            final[i] = total.astype(BF16)
            send(final.at[i], back.at[s], r_send.at[i], r_recv.at[s], at_sp(src))

    stages = (forward, relay, expert, chip_add, finish)

    def step(k, _):
        for lag, stage in enumerate(stages):
            @pl.when((k >= lag) & (k - lag < n))
            def _(stage=stage, lag=lag):
                stage(k - lag)
        return 0

    lax.fori_loop(0, n + len(stages) - 1, step, 0)

    def returned(i, _):
        e = lax.rem(s + i, n)
        landed(back.at[e], r_recv.at[e], at_sp(e))
        return 0

    lax.fori_loop(1, n, returned, 0)

    rows = back[...].reshape(n * cap, width)
    spot = iota((tok, n * cap), 1).astype(F32)
    mixture = jnp.zeros((tok, width), F32)
    for k in range(top):
        pick = (spot == place[k]).astype(F32).astype(BF16)
        mixture = mixture + rw_ref[:, k : k + 1] * dot(pick, rows)
    out_ref[...] = (residual[...].astype(F32) + mixture).astype(BF16)

    for a, source in enumerate((k_ref, v_ref)):
        sent(halo.at[a, 0], halo_send.at[a, 0], right)
        sent(halo.at[a, 1], halo_send.at[a, 1], left)
    sent(part.at[other], ps_send, partner)
    for dy in range(1, ny):
        sent(part_sum.at[dy], py_send.at[dy], partner)
    for dt in range(1, tp):
        sent(squares.at[0], sq_send.at[dt], partner)

    def drain(i, _):
        @pl.when(i > 0)
        def _():
            sent(slots.at[i], d_send.at[i], right)
            sent(final.at[i], r_send.at[i], right)

        sent(final.at[i], fc_send.at[i], partner)
        sent(po_in.at[i], po_send.at[i], partner)
        for dy in range(1, ny):
            sent(final.at[i], fy_send.at[dy, i], partner)
            sent(final.at[i], f2_send.at[dy, i], partner)
            sent(final.at[i], y_send.at[dy, i], partner)
        return 0

    lax.fori_loop(0, n, drain, 0)


def local(
    n, tp,
    queries, key_columns, value_columns, sink_logits, out_weight, stream_in, norm_gain,
    expert_ids, route_weights, gate_weight, up_weight, down_weight,
):
    tok, features = stream_in.shape
    ny = tp // CORES
    cap = 4 * tok // n
    width = features // tp
    hidden = gate_weight.shape[2]
    kv = key_columns.shape[0]
    dma = pltpu.SemaphoreType.DMA
    vmem = pl.BlockSpec(memory_space=pltpu.VMEM)
    hbm = pl.BlockSpec(memory_space=pl.ANY)
    smem = pl.BlockSpec(memory_space=pltpu.SMEM)
    scratch = [
        pltpu.VMEM(out_weight.shape, BF16),
        pltpu.VMEM((tok, width), BF16),
        pltpu.VMEM(gate_weight.shape[1:], BF16),
        pltpu.VMEM(up_weight.shape[1:], BF16),
        pltpu.VMEM(down_weight.shape[1:], BF16),
        pltpu.VMEM((2, 2, kv, WINDOW), BF16),
        pltpu.VMEM(queries.shape, BF16),
        pltpu.VMEM((CORES, ny, tok, width), BF16),
        pltpu.VMEM((ny, tok, width), BF16),
        pltpu.VMEM((ny, tok, width), BF16),
        pltpu.VMEM((ny, tok, width), BF16),
        pltpu.VMEM((tp, 8, tok), F32),
        pltpu.VMEM((n, cap, width), BF16),
        pltpu.VMEM((tp, n, cap, width), BF16),
        pltpu.VMEM((cap, hidden), BF16),
        pltpu.VMEM((n, CORES, ny, cap, width), BF16),
        pltpu.VMEM((n, ny, cap, width), BF16),
        pltpu.VMEM((ny, n, cap, width), BF16),
        pltpu.VMEM((ny, n, cap, width), BF16),
        pltpu.VMEM((n, cap, width), BF16),
        pltpu.VMEM((n, cap, width), BF16),
        pltpu.VMEM((tok, width), BF16),
        dma((5,)),
        dma((2, 2)), dma((2, 2)),
        dma, dma,
        dma((ny,)), dma((ny,)),
        dma((tp,)), dma((tp,)),
        dma((n,)), dma((tp, n)), dma((n,)), dma((ny, n)), dma((ny, n)),
        dma((n,)), dma((n,)),
        dma((ny, n)), dma((ny, n)),
        dma((n,)), dma((n,)),
    ]
    return pl.pallas_call(
        functools.partial(layer, n, tp, cap),
        out_shape=jax.ShapeDtypeStruct((tok, width), BF16),
        in_specs=[vmem, vmem, vmem, smem, vmem, vmem, vmem] + [hbm] * 5,
        out_specs=vmem,
        scratch_shapes=scratch,
        compiler_params=pltpu.CompilerParams(
            collective_id=0, has_side_effects=True, vmem_limit_bytes=60 * 1024 * 1024
        ),
    )(
        queries, key_columns, value_columns, sink_logits, norm_gain[None, :], expert_ids,
        route_weights, out_weight, stream_in, gate_weight, up_weight, down_weight,
    )


def solution(mesh):
    placed = (
        P("sp", "tp"),
        P("tp", "sp"),
        P("tp", "sp"),
        P("tp"),
        P("tp", None),
        P("sp", None),
        P(),
        P("sp", None),
        P("sp", None),
        P("sp", None, "tp"),
        P("sp", None, "tp"),
        P("sp", "tp", None),
    )
    return jax.shard_map(
        functools.partial(local, mesh.shape["sp"], mesh.shape["tp"]),
        mesh=mesh, in_specs=placed, out_specs=P("sp", "tp"), check_vma=False,
    )
```

```python
import functools
import math

import jax
import jax.numpy as jnp
from jax import lax
from jax.experimental import pallas as pl
from jax.experimental.pallas import tpu as pltpu
from jax.sharding import PartitionSpec as P

HD = 64
WINDOW = 128
CORES = 2
EPSILON = 1e-06
MASKED = -1e30
MESH = pl.DeviceIdType.MESH
F32 = jnp.float32
BF16 = jnp.bfloat16


def iota(shape, dim):
    return lax.broadcasted_iota(jnp.int32, shape, dim)


def dot(a, b):
    return jnp.dot(a, b, preferred_element_type=F32)


def as_row(column):
    size = column.shape[0]
    eye = iota((size, size), 0) == iota((size, size), 1)
    return jnp.sum(jnp.where(eye, column, 0.0), axis=0, keepdims=True)


def as_column(row):
    size = row.shape[1]
    eye = iota((size, size), 0) == iota((size, size), 1)
    return jnp.sum(jnp.where(eye, row, 0.0), axis=1, keepdims=True)


def send(src, dst, send_sem, recv_sem, device):
    copy = pltpu.make_async_remote_copy(
        src_ref=src,
        dst_ref=dst,
        send_sem=send_sem,
        recv_sem=recv_sem,
        device_id=device,
        device_id_type=MESH,
    )
    copy.start()


def sent(ref, sem, device):
    pltpu.make_async_remote_copy(
        src_ref=ref, dst_ref=ref, send_sem=sem, recv_sem=sem,
        device_id=device, device_id_type=MESH,
    ).wait_send()


def landed(ref, sem, device):
    pltpu.make_async_remote_copy(
        src_ref=ref, dst_ref=ref, send_sem=sem, recv_sem=sem,
        device_id=device, device_id_type=MESH,
    ).wait_recv()


def layer(
    n, tp, cap,
    q_ref, k_ref, v_ref, sink_ref, gain_ref, ids_ref, rw_ref,
    ow_hbm, stream_hbm, gate_hbm, up_hbm, down_hbm,
    out_ref,
    ow, stream, gate, up, down,
    halo, head, part, part_in, part_sum, part_y, squares,
    slots, xb, hid, po, po_in, chip_sum, sum_y, final, back, residual,
    load_sem, halo_send, halo_recv, ps_send, ps_recv, py_send, py_recv, sq_send, sq_recv,
    d_send, x_recv, fc_send, fy_send, f2_send,
    po_send, po_recv, y_send, y_recv, r_send, r_recv,
):
    s, t = lax.axis_index("sp"), lax.axis_index("tp")
    ny = tp // CORES
    y, c = t // CORES, lax.rem(t, CORES)
    other = 1 - c
    tok, width = residual.shape
    hidden = gate.shape[1]

    def at_sp(i):
        return (i, t)

    def at_tp(j):
        return (s, j)

    partner = at_tp(y * CORES + other)

    def pair(i):
        total, bit = 0, 1
        while bit < n:
            total = total + lax.rem(s // bit + i // bit, 2) * bit
            bit *= 2
        return total

    def peer_y(dy):
        return lax.rem(y + dy, ny)

    def from_y(dy):
        return lax.rem(y + ny - dy, ny)

    loads = [
        pltpu.make_async_copy(ow_hbm, ow, load_sem.at[0]),
        pltpu.make_async_copy(
            stream_hbm.at[:, pl.ds(pl.multiple_of(t * width, 128), width)], stream, load_sem.at[1]
        ),
        pltpu.make_async_copy(gate_hbm.at[0], gate, load_sem.at[2]),
        pltpu.make_async_copy(up_hbm.at[0], up, load_sem.at[3]),
        pltpu.make_async_copy(down_hbm.at[0], down, load_sem.at[4]),
    ]
    for load in loads:
        load.start()

    barrier = pltpu.get_barrier_semaphore()

    def greet_sp(i, _):
        pl.semaphore_signal(
            barrier, inc=1, device_id=at_sp(lax.rem(s + i, n)), device_id_type=MESH
        )
        return 0

    def greet_tp(j, _):
        pl.semaphore_signal(
            barrier, inc=1, device_id=at_tp(lax.rem(t + j, tp)), device_id_type=MESH
        )
        return 0

    lax.fori_loop(1, n, greet_sp, 0)
    lax.fori_loop(1, tp, greet_tp, 0)
    pl.semaphore_wait(barrier, n - 1 + tp - 1)

    right, left = at_sp(lax.rem(s + 1, n)), at_sp(lax.rem(s + n - 1, n))
    for a, source in enumerate((k_ref, v_ref)):
        send(source.at[:, pl.ds(tok - WINDOW, WINDOW)], halo.at[a, 0],
             halo_send.at[a, 0], halo_recv.at[a, 0], right)
        send(source.at[:, pl.ds(0, WINDOW)], halo.at[a, 1],
             halo_send.at[a, 1], halo_recv.at[a, 1], left)

    experts = n
    lanes = iota((tok, 128), 1).astype(F32)
    top = ids_ref.shape[0]
    ids = [as_column(ids_ref[k : k + 1, :].astype(F32)) for k in range(top)]
    hits = [(lanes == ids[k]).astype(F32) for k in range(top)]
    all_hits = functools.reduce(jnp.add, hits)
    before = (iota((tok, tok), 1) < iota((tok, tok), 0)).astype(BF16)
    earlier = dot(before, all_hits.astype(BF16))
    place = [
        jnp.sum(earlier * hits[k], axis=1, keepdims=True) + ids[k] * cap
        for k in range(top)
    ]
    place_row = [as_row(p) for p in place]

    for a, source in enumerate((k_ref, v_ref)):
        landed(halo.at[a, 0], halo_recv.at[a, 0], left)
        landed(halo.at[a, 1], halo_recv.at[a, 1], right)

    kv_heads = k_ref.shape[0] // HD
    group = q_ref.shape[1] // HD // kv_heads
    span = 3 * WINDOW
    row = lax.rem(iota((group * WINDOW, span), 0), WINDOW)
    col = iota((group * WINDOW, span), 1)
    near = (col - row >= 0) & (col - row <= 2 * WINDOW)
    for b in range(tok // WINDOW):
        key_pos = s * tok + (b - 1) * WINDOW + col
        visible = near & (key_pos >= 0) & (key_pos < n * tok)
        rows = pl.ds(b * WINDOW, WINDOW)
        for g in range(kv_heads):
            feats = pl.ds(g * HD, HD)
            kx, vx = [
                jnp.concatenate(
                    [halo[a, 0, feats, :], ref[feats, :], halo[a, 1, feats, :]], axis=1
                )[:, b * WINDOW : b * WINDOW + span]
                for a, ref in enumerate((k_ref, v_ref))
            ]
            qs = jnp.concatenate(
                [q_ref[rows, pl.ds((g * group + h) * HD, HD)] for h in range(group)], axis=0
            )
            sink = jnp.concatenate(
                [jnp.full((WINDOW, 1), sink_ref[g * group + h], F32) for h in range(group)], axis=0
            )
            scores = jnp.where(visible, dot(qs, kx) * (1.0 / math.sqrt(HD)), MASKED)
            row_top = jnp.maximum(jnp.max(scores, axis=1, keepdims=True), sink)
            weight = jnp.where(visible, jnp.exp(scores - row_top), 0.0)
            total = jnp.sum(weight, axis=1, keepdims=True) + jnp.exp(sink - row_top)
            weight = (weight * (1.0 / total)).astype(BF16)
            mixed = lax.dot_general(
                weight, vx, (((1,), (1,)), ((), ())), preferred_element_type=F32
            ).astype(BF16)
            head[rows, pl.ds(g * group * HD, group * HD)] = jnp.concatenate(
                [mixed[h * WINDOW : (h + 1) * WINDOW] for h in range(group)], axis=1
            )

    loads[0].wait()
    loads[1].wait()

    def project(core):
        for yy in range(ny):
            start = pl.multiple_of((yy * CORES + core) * width, 128)
            part[core, yy] = dot(head[...], ow[:, pl.ds(start, width)]).astype(BF16)

    project(other)
    send(part.at[other], part_in, ps_send, ps_recv, partner)
    project(c)
    landed(part_in, ps_recv, partner)
    for dy in range(1, ny):
        yy = peer_y(dy)
        part_sum[dy] = (part[c, yy].astype(F32) + part_in[yy].astype(F32)).astype(BF16)
        send(part_sum.at[dy], part_y.at[dy], py_send.at[dy], py_recv.at[dy],
             at_tp(yy * CORES + c))
    attn = part[c, y].astype(F32) + part_in[y].astype(F32)
    for dy in range(1, ny):
        landed(part_y.at[dy], py_recv.at[dy], at_tp(from_y(dy) * CORES + c))
        attn = attn + part_y[dy].astype(F32)
    res = (stream[...].astype(F32) + attn.astype(BF16).astype(F32)).astype(BF16)
    residual[...] = res
    res = res.astype(F32)
    own_squares = jnp.broadcast_to(as_row(jnp.sum(res * res, axis=1, keepdims=True)), (8, tok))
    squares[0] = own_squares
    for dt in range(1, tp):
        send(squares.at[0], squares.at[dt], sq_send.at[dt], sq_recv.at[dt],
             at_tp(lax.rem(t + dt, tp)))
    square_sum = own_squares
    for dt in range(1, tp):
        landed(squares.at[dt], sq_recv.at[dt], at_tp(lax.rem(t + tp - dt, tp)))
        square_sum = square_sum + squares[dt]
    inverse = as_column(lax.rsqrt(square_sum[0:1] / (tp * width) + EPSILON))
    gain = gain_ref[:, pl.ds(pl.multiple_of(t * width, 128), width)]
    normed = (res * inverse * gain).astype(BF16)

    slot = iota((cap, tok), 0)

    def rows_of(e):
        wanted = (slot + e * cap).astype(F32)
        pick = functools.reduce(jnp.logical_or, [wanted == p for p in place_row])
        return dot(pick.astype(F32).astype(BF16), normed).astype(BF16)

    xb[t, s] = rows_of(s)

    def dispatch(i, _):
        e = pair(i)
        slots[i] = rows_of(e)
        send(slots.at[i], xb.at[t, s], d_send.at[i], x_recv.at[t, s], at_sp(e))
        return 0

    lax.fori_loop(1, n, dispatch, 0)
    for load in loads[2:]:
        load.wait()

    def forward(i):
        src = pair(i)

        @pl.when(i > 0)
        def _():
            landed(xb.at[t, src], x_recv.at[t, src], at_sp(src))

        for dy in range(1, ny):
            send(xb.at[t, src], xb.at[t, src], fy_send.at[dy, i], x_recv.at[t, src],
                 at_tp(peer_y(dy) * CORES + c))
        send(xb.at[t, src], xb.at[t, src], fc_send.at[i], x_recv.at[t, src], partner)

    def relay(i):
        src = pair(i)
        for dy in range(1, ny):
            j = from_y(dy) * CORES + c
            landed(xb.at[j, src], x_recv.at[j, src], at_tp(j))
            send(xb.at[j, src], xb.at[j, src], f2_send.at[dy, i], x_recv.at[j, src], partner)

    tile = min(hidden, 256)

    def expert(i):
        src = pair(i)
        for yy in range(ny):
            j = yy * CORES + other
            landed(xb.at[j, src], x_recv.at[j, src], partner)
        rows = jnp.concatenate([xb[j, src] for j in range(tp)], axis=1)
        for f in range(hidden // tile):
            cols = pl.ds(f * tile, tile)
            gate_pre = dot(rows, gate[:, cols])
            upward = dot(rows, up[:, cols])
            hid[:, cols] = (gate_pre / (1.0 + jnp.exp(-gate_pre)) * upward).astype(BF16)
        for j in range(tp):
            po[i, j % CORES, j // CORES] = dot(
                hid[...], down[:, j * width : (j + 1) * width]
            ).astype(BF16)
        send(po.at[i, other], po_in.at[i], po_send.at[i], po_recv.at[i], partner)

    def chip_add(i):
        landed(po_in.at[i], po_recv.at[i], partner)
        for dy in range(1, ny):
            yy = peer_y(dy)
            chip_sum[dy, i] = (po[i, c, yy].astype(F32) + po_in[i, yy].astype(F32)).astype(BF16)
            send(chip_sum.at[dy, i], sum_y.at[dy, i], y_send.at[dy, i], y_recv.at[dy, i],
                 at_tp(yy * CORES + c))

    def finish(i):
        src = pair(i)
        total = po[i, c, y].astype(F32) + po_in[i, y].astype(F32)
        for dy in range(1, ny):
            landed(sum_y.at[dy, i], y_recv.at[dy, i], at_tp(from_y(dy) * CORES + c))
            total = total + sum_y[dy, i].astype(F32)

        @pl.when(i == 0)
        def _():
            back[s] = total.astype(BF16)

        @pl.when(i > 0)
        def _():
            final[i] = total.astype(BF16)
            send(final.at[i], back.at[s], r_send.at[i], r_recv.at[s], at_sp(src))

    stages = (forward, relay, expert, chip_add, finish)

    def step(k, _):
        for lag, stage in reversed(tuple(enumerate(stages))):
            @pl.when((k >= lag) & (k - lag < n))
            def _(stage=stage, lag=lag):
                stage(k - lag)
        return 0

    lax.fori_loop(0, n + len(stages) - 1, step, 0)

    def returned(i, _):
        e = lax.rem(s + i, n)
        landed(back.at[e], r_recv.at[e], at_sp(e))
        return 0

    lax.fori_loop(1, n, returned, 0)

    rows = back[...].reshape(n * cap, width)
    spot = iota((tok, n * cap), 1).astype(F32)
    mixture = jnp.zeros((tok, width), F32)
    for k in range(top):
        pick = (spot == place[k]).astype(F32).astype(BF16)
        mixture = mixture + as_column(rw_ref[k : k + 1, :]) * dot(pick, rows)
    out_ref[...] = (residual[...].astype(F32) + mixture).astype(BF16)

    for a, source in enumerate((k_ref, v_ref)):
        sent(halo.at[a, 0], halo_send.at[a, 0], right)
        sent(halo.at[a, 1], halo_send.at[a, 1], left)
    sent(part.at[other], ps_send, partner)
    for dy in range(1, ny):
        sent(part_sum.at[dy], py_send.at[dy], partner)
    for dt in range(1, tp):
        sent(squares.at[0], sq_send.at[dt], partner)

    def drain(i, _):
        @pl.when(i > 0)
        def _():
            sent(slots.at[i], d_send.at[i], right)
            sent(final.at[i], r_send.at[i], right)

        sent(final.at[i], fc_send.at[i], partner)
        sent(po_in.at[i], po_send.at[i], partner)
        for dy in range(1, ny):
            sent(final.at[i], fy_send.at[dy, i], partner)
            sent(final.at[i], f2_send.at[dy, i], partner)
            sent(final.at[i], y_send.at[dy, i], partner)
        return 0

    lax.fori_loop(0, n, drain, 0)


def local(
    n, tp,
    queries, key_columns, value_columns, sink_logits, out_weight, stream_in, norm_gain,
    expert_ids, route_weights, gate_weight, up_weight, down_weight,
):
    tok, features = stream_in.shape
    ny = tp // CORES
    cap = 4 * tok // n
    width = features // tp
    hidden = gate_weight.shape[2]
    kv = key_columns.shape[0]
    dma = pltpu.SemaphoreType.DMA
    vmem = pl.BlockSpec(memory_space=pltpu.VMEM)
    hbm = pl.BlockSpec(memory_space=pl.ANY)
    smem = pl.BlockSpec(memory_space=pltpu.SMEM)
    scratch = [
        pltpu.VMEM(out_weight.shape, BF16),
        pltpu.VMEM((tok, width), BF16),
        pltpu.VMEM(gate_weight.shape[1:], BF16),
        pltpu.VMEM(up_weight.shape[1:], BF16),
        pltpu.VMEM(down_weight.shape[1:], BF16),
        pltpu.VMEM((2, 2, kv, WINDOW), BF16),
        pltpu.VMEM(queries.shape, BF16),
        pltpu.VMEM((CORES, ny, tok, width), BF16),
        pltpu.VMEM((ny, tok, width), BF16),
        pltpu.VMEM((ny, tok, width), BF16),
        pltpu.VMEM((ny, tok, width), BF16),
        pltpu.VMEM((tp, 8, tok), F32),
        pltpu.VMEM((n, cap, width), BF16),
        pltpu.VMEM((tp, n, cap, width), BF16),
        pltpu.VMEM((cap, hidden), BF16),
        pltpu.VMEM((n, CORES, ny, cap, width), BF16),
        pltpu.VMEM((n, ny, cap, width), BF16),
        pltpu.VMEM((ny, n, cap, width), BF16),
        pltpu.VMEM((ny, n, cap, width), BF16),
        pltpu.VMEM((n, cap, width), BF16),
        pltpu.VMEM((n, cap, width), BF16),
        pltpu.VMEM((tok, width), BF16),
        dma((5,)),
        dma((2, 2)), dma((2, 2)),
        dma, dma,
        dma((ny,)), dma((ny,)),
        dma((tp,)), dma((tp,)),
        dma((n,)), dma((tp, n)), dma((n,)), dma((ny, n)), dma((ny, n)),
        dma((n,)), dma((n,)),
        dma((ny, n)), dma((ny, n)),
        dma((n,)), dma((n,)),
    ]
    return pl.pallas_call(
        functools.partial(layer, n, tp, cap),
        out_shape=jax.ShapeDtypeStruct((tok, width), BF16),
        in_specs=[vmem, vmem, vmem, smem, vmem, vmem, vmem] + [hbm] * 5,
        out_specs=vmem,
        scratch_shapes=scratch,
        compiler_params=pltpu.CompilerParams(
            collective_id=0, has_side_effects=True, vmem_limit_bytes=60 * 1024 * 1024
        ),
    )(
        queries, key_columns, value_columns, sink_logits, norm_gain[None, :], expert_ids.T,
        route_weights.T, out_weight, stream_in, gate_weight, up_weight, down_weight,
    )


def solution(mesh):
    placed = (
        P("sp", "tp"),
        P("tp", "sp"),
        P("tp", "sp"),
        P("tp"),
        P("tp", None),
        P("sp", None),
        P(),
        P("sp", None),
        P("sp", None),
        P("sp", None, "tp"),
        P("sp", None, "tp"),
        P("sp", "tp", None),
    )
    return jax.shard_map(
        functools.partial(local, mesh.shape["sp"], mesh.shape["tp"]),
        mesh=mesh, in_specs=placed, out_specs=P("sp", "tp"), check_vma=False,
    )
```
